256 devices in a mesh: sp: 16 (over y, x), dp: 16 (over z, core).
Axes of the slice: x: 4, y: 4, z: 8, core: 2. Of those that a mesh axis runs over, the one named last changes fastest.
Arguments:
- tokens: bfloat16 [16, 2048, 2048], P('dp', 'sp'), may hold values from -6 to 6
- query_weight: bfloat16 [2048, 1024], P('dp'), may hold values from -0.125 to 0.125
- key_weight: bfloat16 [2048, 1024], P('dp'), may hold values from -0.125 to 0.125
- value_weight: bfloat16 [2048, 2048], P('dp'), may hold values from -0.125 to 0.125
- output_weight: bfloat16 [2048, 2048], P('dp'), may hold values from -0.125 to 0.125
- log_decay: float32 [2, 16], P(None, 'sp'), may hold values from -0.04 to 0, as said below
Outputs:
- mixed: bfloat16 [16, 2048, 2048], P('dp', 'sp')
The draws below stay inside these ranges and needn't reach their ends.
Inputs may be any that keep to these rules, and one draw needn't show every extreme that they name: `log_decay`: every entry is negative: the logarithm of a head's decay per position.
All inputs are finite; a program needn't handle non-finite values.
Results may differ from the reference program's by a relative error of at most 0.012.
Values may be sent and summed in bfloat16 or wider, within the bound.
No kernel may reach another device: no remote copies, remote signals or barrier semaphores. Data moves between devices by JAX's collectives and lax.ppermute only.
A program may use at most 128 MiB of HBM per device.

```python
import jax
import jax.numpy as jnp
from jax import lax

D = 2048
HEADS = 16
DK = 64
DV = 128
BLOCK = 512
SEQ = 2048
SEQS = 16


def draw_log_decay(key, part):
    first_key, second_key, third_key = jax.random.split(jax.random.fold_in(key, 17), 3)
    share = 0.5
    fast = jax.random.uniform(first_key, (2, HEADS), jnp.float32) < share
    fast_rate = jnp.exp(jax.random.uniform(second_key, (2, HEADS), jnp.float32, jnp.log(1.0 / 80.0), jnp.log(1.0 / 25.0)))
    slow_rate = jax.random.uniform(third_key, (2, HEADS), jnp.float32, 0.3, 2.0) / SEQ
    return (-jnp.where(fast, fast_rate, slow_rate)).astype(jnp.float32)


def level_of(rng, dims, shards, smallest, largest):
    factor_of, own = 1.0, jax.random.fold_in(rng, 6)
    for axis_at, shards_of in shards:
        draws = jnp.exp(jax.random.uniform(jax.random.fold_in(own, axis_at), (shards_of,), jnp.float32, smallest / len(shards), largest / len(shards)))
        factor_of = factor_of * jnp.repeat(draws, dims[axis_at] // shards_of).reshape([-1 if axis == axis_at else 1 for axis in range(len(dims))])
    return factor_of


def gaussian(key, extent, deviation, bound, cuts=(), kind=jnp.bfloat16):
    values = deviation * jax.random.normal(key, extent, jnp.float32)
    if cuts:
        values = values * level_of(key, extent, cuts, -0.22, 0.18)
    return jnp.clip(values, -bound, bound).astype(kind)


def setup_inputs(seed: int = 0) -> dict:
    splits = jax.random.split(jax.random.key(seed), 7)
    return {
        "tokens": gaussian(splits[0], (SEQS, SEQ, D), 1.0, 6.0, ((0, 16), (1, 16))),
        "query_weight": gaussian(splits[1], (D, HEADS * DK), D ** -0.5, 0.125, ((0, 16),)),
        "key_weight": gaussian(splits[2], (D, HEADS * DK), D ** -0.5, 0.125, ((0, 16),)),
        "value_weight": gaussian(splits[3], (D, HEADS * DV), D ** -0.5, 0.125, ((0, 16),)),
        "output_weight": gaussian(splits[4], (HEADS * DV, D), (HEADS * DV) ** -0.5, 0.125, ((0, 16),)),
        "log_decay": draw_log_decay(jax.random.fold_in(splits[6], 71), 0),
    }


exact_precision = lax.Precision.HIGHEST

def rotate(values_part, positions):
    half_dim = values_part.shape[-1] // 2
    frequency = 10000.0 ** (-jnp.arange(half_dim, dtype=jnp.float32) / half_dim)
    angles = positions[:, None] * frequency[None, :]
    cosine = jnp.cos(angles)[:, None, :]
    sine_part = jnp.sin(angles)[:, None, :]
    first = values_part[..., :half_dim]
    second = values_part[..., half_dim:]
    return jnp.concatenate([first * cosine - second * sine_part, first * sine_part + second * cosine], axis=-1)

def retain(query, key_rows, value_rows, log_rate):
    length, heads, key_dim = query.shape
    value_dim = value_rows.shape[-1]
    count = length // BLOCK
    offsets = jnp.arange(BLOCK, dtype=jnp.float32)
    distance = offsets[:, None] - offsets[None, :]
    decay_inner = jnp.where(distance[None] >= 0.0, jnp.exp(log_rate[:, None, None] * jnp.maximum(distance, 0.0)[None]), 0.0)
    decay_query = jnp.exp((offsets[:, None] + 1.0) * log_rate[None, :])[:, :, None]
    decay_key = jnp.exp((BLOCK - 1.0 - offsets)[:, None] * log_rate[None, :])[:, :, None]
    decay_block = jnp.exp(BLOCK * log_rate)[:, None, None]

    def blocks(array):
        return array.reshape(count, BLOCK, heads, array.shape[-1])

    def advance(state, inputs):
        query_block, key_block, value_block = inputs
        query_wide = query_block.astype(jnp.float32)
        key_wide = key_block.astype(jnp.float32)
        value_wide = value_block.astype(jnp.float32)
        inner = jnp.einsum('ihd,jhd->hij', query_wide, key_wide, precision=exact_precision) * decay_inner
        inner = inner.astype(jnp.bfloat16).astype(jnp.float32)
        result = jnp.einsum('hij,jhv->ihv', inner, value_wide, precision=exact_precision)
        result = result + jnp.einsum('ihd,hdv->ihv', query_wide * decay_query, state, precision=exact_precision)
        state = state * decay_block + jnp.einsum('jhd,jhv->hdv', key_wide * decay_key, value_wide, precision=exact_precision)
        return (state, result)
    initial = jnp.zeros((heads, key_dim, value_dim), jnp.float32)
    final_state, outputs = lax.scan(advance, initial, (blocks(query), blocks(key_rows), blocks(value_rows)))
    return outputs.reshape(length, heads, value_dim)

def mechanism(stacked, log_decay):
    length = stacked.shape[0]
    widened = stacked[..., :2 * DK].astype(jnp.float32)
    positions = jnp.arange(length, dtype=jnp.float32)
    query = rotate(widened[..., :DK], positions).astype(jnp.bfloat16)
    key_rows = rotate(widened[..., DK:2 * DK], positions).astype(jnp.bfloat16)
    value_rows = stacked[..., 2 * DK:]
    forward = retain(query, key_rows, value_rows, log_decay[0])
    backward = retain(jnp.flip(query, 0), jnp.flip(key_rows, 0), jnp.flip(value_rows, 0), log_decay[1])
    combined = forward + jnp.flip(backward, 0)
    average = lax.optimization_barrier(jnp.mean(combined, axis=-1, keepdims=True))
    centred = combined - average
    variance = lax.optimization_barrier(jnp.mean(centred * centred, axis=-1, keepdims=True))
    return (centred * lax.rsqrt(variance + 1e-06)).astype(jnp.bfloat16)

def reference(tokens, query_weight, key_weight, value_weight, output_weight, log_decay):

    def one_sequence(rows):
        length = rows.shape[0]
        query = jnp.dot(rows, query_weight, preferred_element_type=jnp.float32).astype(jnp.bfloat16).reshape(length, HEADS, DK)
        key_rows = jnp.dot(rows, key_weight, preferred_element_type=jnp.float32).astype(jnp.bfloat16).reshape(length, HEADS, DK)
        value_rows = jnp.dot(rows, value_weight, preferred_element_type=jnp.float32).astype(jnp.bfloat16).reshape(length, HEADS, DV)
        stacked = jnp.concatenate([query, key_rows, value_rows], axis=2)
        normed = mechanism(stacked, log_decay).reshape(length, HEADS * DV)
        return jnp.dot(normed, output_weight, preferred_element_type=jnp.float32).astype(jnp.bfloat16)
    return lax.map(one_sequence, tokens)
```

```python
import functools

import jax
import jax.numpy as jnp
from jax import lax
from jax.experimental import pallas as pl
from jax.experimental.pallas import tpu as pltpu
from jax.sharding import Mesh, PartitionSpec as P

DK = 64
DV = 128
BLOCK = 512
GROUP = 4
SUB = 128
NX = 4
NY = 4
NZ = 8
WIDTH = GROUP * (2 * DK + DV)
VM = pl.BlockSpec(memory_space=pltpu.VMEM)
SM = pl.BlockSpec(memory_space=pltpu.SMEM)
f32 = jnp.float32
bf16 = jnp.bfloat16


def dot(a, b, dims=(((1,), (0,)), ((), ()))):
    return lax.dot_general(a, b, dims, preferred_element_type=f32)


def by_shift(array, axis, shift):
    count = lax.axis_size(axis)
    return lax.ppermute(array, axis, [(i, (i + shift) % count) for i in range(count)])


def swap_cores(array):
    return lax.ppermute(array, "c", [(0, 1), (1, 0)])


def ring_step(array):
    pairs = []
    for z in range(NZ):
        pairs.append((2 * z, 2 * ((z + 1) % NZ)))
        pairs.append((2 * z + 1, 2 * ((z - 1) % NZ) + 1))
    return lax.ppermute(array, ("z", "c"), pairs)


def out_rows_spread(array):
    pairs = []
    for y in range(NY):
        for x in range(NX):
            for z in range(NZ):
                to = (z + x + 4 * (y % 2)) % NZ
                pairs.append(((y * NX + x) * NZ + z, (y * NX + x) * NZ + to))
    return lax.ppermute(array, ("y", "x", "z"), pairs)


def out_rows_fetch(array, turn):
    pairs = []
    for y in range(NY):
        for x in range(NX):
            for z in range(NZ):
                held = (z - x - 4 * (y % 2)) % NZ
                to_x, part = held // 2, held % 2
                to_y = 2 * (y // 2) + (part - turn) % 2
                pairs.append(((y * NX + x) * NZ + z, (to_y * NX + to_x) * NZ + z))
    return lax.ppermute(array, ("y", "x", "z"), pairs)


def project_kernel(
    place, rates, t0, t1, t2, t3, w0, a1, b1, a2, b2, a3, b3, a4, b4, cosine, sine,
    rq_out, rk_out, v_out, s1_out, s2_out, s3_out, rows, acc,
):
    y, x, z, c = place[0], place[1], place[2], place[3]
    for shift, part in enumerate((t0, t1, t2, t3)):
        at = lax.rem(x - shift + NX, NX)
        rows[pl.ds(at * SUB, SUB), :] = part[...]
    sign = 1 - 2 * c

    def of_z(distance):
        return lax.rem(z + distance + 2 * NZ, NZ)

    pairs = (
        (w0, of_z(0)),
        (a1, of_z(-sign)), (b1, of_z(sign)),
        (a2, of_z(-2 * sign)), (b2, of_z(2 * sign)),
        (a3, of_z(-3 * sign)), (b3, of_z(3 * sign)),
    )
    for n, (weight, at) in enumerate(pairs):
        part = dot(rows[:, pl.ds(at * 256, 256)], weight[...])
        if n == 0:
            acc[...] = part
        else:
            acc[...] += part
    far = of_z(4)
    acc[...] += dot(rows[:, pl.ds((2 * far + c) * 128, 128)], a4[...])
    acc[...] += dot(rows[:, pl.ds((2 * far + 1 - c) * 128, 128)], b4[...])

    half = DK // 2
    row = lax.broadcasted_iota(jnp.int32, (128, 128), 0)
    col = lax.broadcasted_iota(jnp.int32, (128, 128), 1)
    first = lax.rem(col, DK) < half
    turn = jnp.where(
        first & (row == col + half), -1.0, jnp.where((~first) & (row == col - half), 1.0, 0.0)
    ).astype(bf16)
    spot = lax.broadcasted_iota(jnp.int32, (BLOCK, 128), 0).astype(f32)
    lane = lax.broadcasted_iota(jnp.int32, (BLOCK, 128), 1)
    values = acc[:, 2 * GROUP * DK :].astype(bf16)
    v_out[...] = values
    for pair in range(GROUP // 2):
        for at, out in ((0, rq_out), (GROUP * DK, rk_out)):
            part = acc[:, at + pair * 128 : at + (pair + 1) * 128].astype(bf16)
            turned = part.astype(f32) * cosine[...] + dot(part, turn) * sine[...]
            out[:, pair * 128 : (pair + 1) * 128] = turned.astype(bf16)
        keys = turned.astype(bf16).astype(f32)
        rate_f = jnp.where(lane < DK, rates[0, 2 * pair], rates[0, 2 * pair + 1])
        rate_b = jnp.where(lane < DK, rates[1, 2 * pair], rates[1, 2 * pair + 1])
        keys_f = (keys * jnp.exp(rate_f * (BLOCK - 1.0 - spot))).astype(bf16)
        keys_b = (keys * jnp.exp(rate_b * spot)).astype(bf16)
        two = values[:, pair * 2 * DV : (pair + 1) * 2 * DV]
        state_f = dot(keys_f, two, (((0,), (0,)), ((), ()))).astype(bf16)
        state_b = dot(keys_b, two, (((0,), (0,)), ((), ()))).astype(bf16)
        for h in range(2):
            into = pl.ds((2 * pair + h) * DK, DK)
            fwd = state_f[h * DK : (h + 1) * DK, h * DV : (h + 1) * DV]
            bwd = state_b[h * DK : (h + 1) * DK, h * DV : (h + 1) * DV]
            for shift, out in ((1, s1_out), (2, s2_out), (3, s3_out)):
                out[into, :] = jnp.where(y + shift < NY, fwd, bwd)


def retain_kernel(
    place, rates, rq, rk, values, r1, r2, r3, wa0, wa1, wb0, wb1, out, normed, *, shift
):
    y, x, c = place[0], place[1], place[3]
    at = lax.rem(x + shift, NX)
    start = at * SUB
    query_at = lax.broadcasted_iota(jnp.int32, (SUB, BLOCK), 0) + start
    key_at = lax.broadcasted_iota(jnp.int32, (SUB, BLOCK), 1)
    gap = (query_at - key_at).astype(f32)
    spot = (lax.broadcasted_iota(jnp.int32, (SUB, DV), 0) + start).astype(f32)
    ones = jnp.ones((DK, DV), f32)
    for h in range(GROUP):
        rate_f, rate_b = rates[0, h], rates[1, h]
        decay = jnp.exp(jnp.where(gap >= 0.0, rate_f * gap, -rate_b * gap))
        decay = jnp.where(gap == 0.0, 2.0, decay)
        query = rq[pl.ds(start, SUB), h * DK : (h + 1) * DK]
        key = rk[:, h * DK : (h + 1) * DK]
        scores = (dot(query, key, (((1,), (1,)), ((), ()))) * decay).astype(bf16)
        result = dot(scores, values[:, h * DV : (h + 1) * DV])
        state_f = jnp.zeros((DK, DV), f32)
        state_b = jnp.zeros((DK, DV), f32)
        for k, got in ((1, r1), (2, r2), (3, r3)):
            state = got[h * DK : (h + 1) * DK, :].astype(f32)
            ahead = y >= k
            state_f += jnp.where(ahead, state * jnp.exp(ones * (rate_f * (BLOCK * (k - 1.0)))), 0.0)
            state_b += jnp.where(ahead, 0.0, state * jnp.exp(ones * (rate_b * (BLOCK * (3.0 - k)))))
        result += jnp.exp(rate_f * (spot + 1.0)) * dot(query, state_f.astype(bf16))
        result += jnp.exp(rate_b * (BLOCK - spot)) * dot(query, state_b.astype(bf16))
        average = jnp.mean(result, axis=-1, keepdims=True)
        centred = result - average
        variance = jnp.mean(centred * centred, axis=-1, keepdims=True)
        normed[h] = (centred * lax.rsqrt(variance + 1e-06)).astype(bf16)
    first = lax.rem(y, 2)
    second = 1 - first
    total = dot(normed[2 * first + c], wa0[...])
    total += dot(normed[2 * second + c], wa1[...])
    total += dot(normed[2 * first + 1 - c], wb0[...])
    total += dot(normed[2 * second + 1 - c], wb1[...])
    out[...] = total.astype(out.dtype)


def shards(tokens, query_weight, key_weight, value_weight, output_weight, log_decay):
    y, x, z, c = (lax.axis_index(a) for a in ("y", "x", "z", "c"))
    place = jnp.stack([y, x, z, c]).astype(jnp.int32)
    t0 = tokens[0]
    t2, t1, t3 = (by_shift(t0, "x", k) for k in (2, 1, 3))

    own = jnp.concatenate(
        [
            lax.dynamic_slice_in_dim(query_weight, x * GROUP * DK, GROUP * DK, 1),
            lax.dynamic_slice_in_dim(key_weight, x * GROUP * DK, GROUP * DK, 1),
            lax.dynamic_slice_in_dim(value_weight, x * GROUP * DV, GROUP * DV, 1),
        ],
        axis=1,
    )
    other = swap_cores(own)
    w0 = jnp.where(c == 0, jnp.concatenate([own, other]), jnp.concatenate([other, own]))
    a1 = ring_step(w0)
    a2 = ring_step(a1)
    a3 = ring_step(a2)
    a4 = ring_step(lax.dynamic_slice_in_dim(a3, c * 128, 128, 0))
    b1, b2, b3, b4 = (swap_cores(a) for a in (a1, a2, a3, a4))

    spread = out_rows_spread(lax.optimization_barrier((output_weight, a3))[0])
    wa0, wa1 = (out_rows_fetch(spread, turn) for turn in (0, 1))
    wb0, wb1 = (swap_cores(a) for a in (wa0, wa1))

    rates = lax.all_gather(log_decay, ("y", "x"), axis=1, tiled=True)
    rates = lax.dynamic_slice_in_dim(rates, x * GROUP, GROUP, 1)
    half = DK // 2
    frequency = 10000.0 ** (-jnp.arange(half, dtype=f32) / half)
    positions = (y * BLOCK + jnp.arange(BLOCK)).astype(f32)
    angles = positions[:, None] * frequency[None, :]
    cosine = jnp.tile(jnp.cos(angles), (1, 4))
    sine = jnp.tile(jnp.sin(angles), (1, 4))

    state = jax.ShapeDtypeStruct((GROUP * DK, DV), bf16)
    rq, rk, values, s1, s2, s3 = pl.pallas_call(
        project_kernel,
        out_shape=(
            jax.ShapeDtypeStruct((BLOCK, GROUP * DK), bf16),
            jax.ShapeDtypeStruct((BLOCK, GROUP * DK), bf16),
            jax.ShapeDtypeStruct((BLOCK, GROUP * DV), bf16),
            state, state, state,
        ),
        in_specs=[SM, SM] + [VM] * 15,
        out_specs=[VM] * 6,
        scratch_shapes=[
            pltpu.VMEM((BLOCK, t0.shape[1]), bf16),
            pltpu.VMEM((BLOCK, WIDTH), f32),
        ],
        name="project",
    )(place, rates, t0, t1, t2, t3, w0, a1, b1, a2, b2, a3, b3, a4, b4, cosine, sine)
    r1, r2, r3 = (by_shift(s, "y", k) for k, s in ((1, s1), (2, s2), (3, s3)))

    def part_for(shift, kind):
        return pl.pallas_call(
            functools.partial(retain_kernel, shift=shift),
            out_shape=jax.ShapeDtypeStruct((SUB, output_weight.shape[1]), kind),
            in_specs=[SM, SM] + [VM] * 10,
            out_specs=VM,
            scratch_shapes=[pltpu.VMEM((GROUP, SUB, DV), bf16)],
            name="retain",
        )(place, rates, rq, rk, values, r1, r2, r3, wa0, wa1, wb0, wb1)

    sent = [by_shift(part_for(shift, bf16), "x", shift) for shift in (2, 1, 3)]
    total = part_for(0, f32)
    for part in sent:
        total = total + part.astype(f32)
    return total.astype(bf16)[None]


def solution(mesh):
    finer = Mesh(mesh.devices.reshape(NY, NX, NZ, 2), ("y", "x", "z", "c"))
    dp, sp = ("z", "c"), ("y", "x")
    placed = (P(dp, sp, None), P(dp, None), P(dp, None), P(dp, None), P(dp, None), P(None, sp))
    return jax.shard_map(
        shards, mesh=finer, in_specs=placed, out_specs=P(dp, sp, None), check_vma=False
    )
```

```python
import functools

import jax
import jax.numpy as jnp
from jax import lax
from jax.experimental import pallas as pl
from jax.experimental.pallas import tpu as pltpu
from jax.sharding import Mesh, PartitionSpec as P

DK = 64
DV = 128
BLOCK = 512
GROUP = 4
SUB = 128
CHUNKS = BLOCK // SUB
NX = 4
NY = 4
NZ = 8
WIDTH = GROUP * (2 * DK + DV)
VM = pl.BlockSpec(memory_space=pltpu.VMEM)
ANY = pl.BlockSpec(memory_space=pltpu.HBM)
SM = pl.BlockSpec(memory_space=pltpu.SMEM)
f32 = jnp.float32
bf16 = jnp.bfloat16


def dot(a, b, dims=(((1,), (0,)), ((), ()))):
    return lax.dot_general(a, b, dims, preferred_element_type=f32)


def in_vmem(*arrays):
    return tuple(pltpu.with_memory_space_constraint(a, pltpu.VMEM) for a in arrays)


def by_shift(array, axis, shift):
    count = lax.axis_size(axis)
    return lax.ppermute(array, axis, [(i, (i + shift) % count) for i in range(count)])


def swap_cores(array):
    return lax.ppermute(array, "c", [(0, 1), (1, 0)])


def out_rows_spread(array):
    pairs = []
    for y in range(NY):
        for x in range(NX):
            for z in range(NZ):
                for c in range(2):
                    to = (z + x + 4 * (y % 2) + 4 * c) % NZ
                    at = (y * NX + x) * NZ
                    pairs.append(((at + z) * 2 + c, (at + to) * 2 + c))
    return lax.ppermute(array, ("y", "x", "z", "c"), pairs)


def out_rows_fetch(array):
    pairs = []
    for y in range(NY):
        for x in range(NX):
            for z in range(NZ):
                for c in range(2):
                    gone = (z - (2 * y + x // 2) - 4 * (x % 2)) % NZ
                    from_x, from_y = gone % 4, gone // 4 + 2 * c
                    source = ((from_y * NX + from_x) * NZ + z) * 2 + x % 2
                    pairs.append((source, ((y * NX + x) * NZ + z) * 2 + c))
    return lax.ppermute(array, ("y", "x", "z", "c"), sorted(pairs))


def pack_kernel(place, query_in, key_in, value_in, rows_in, out, rows, query, key, value, sems):
    y, x = place[0], place[1]
    part = pl.ds(pl.multiple_of((y // 2) * rows.shape[1], 128), rows.shape[1])
    copies = [pltpu.make_async_copy(rows_in.at[:, part], rows, sems.at[12])]
    for j in range(GROUP):
        along = pl.ds(j * 128, 128)
        narrow = pl.ds(pl.multiple_of((2 * j + x // 2) * 128, 128), 128)
        wide = pl.ds(pl.multiple_of((4 * j + x) * DV, 128), DV)
        for n, (source, columns, to) in enumerate(
            ((query_in, narrow, query), (key_in, narrow, key), (value_in, wide, value))
        ):
            copies.append(
                pltpu.make_async_copy(source.at[:, columns], to.at[:, along], sems.at[3 * j + n])
            )
    for copy in copies:
        copy.start()
    for copy in copies:
        copy.wait()
    lane = lax.broadcasted_iota(jnp.int32, (SUB, 128), 1)
    odd = lax.rem(x, 2) == 1
    for n, source in enumerate((query, key)):
        for pair in range(GROUP // 2):
            low = source[:, 2 * pair * 128 : (2 * pair + 1) * 128].astype(f32)
            high = source[:, (2 * pair + 1) * 128 : (2 * pair + 2) * 128].astype(f32)
            low_to = jnp.where(odd, pltpu.roll(low, DK, 1), low)
            high_to = jnp.where(odd, high, pltpu.roll(high, DK, 1))
            at = n * GROUP * DK + pair * 128
            out[:, at : at + 128] = jnp.where(lane < DK, low_to, high_to).astype(bf16)
    out[:, 2 * GROUP * DK :] = value[...]


def project_kernel(
    place, rates, t0, t1, t2, t3, own, f1, b1, f2, b2, f3, b3, f4, b4,
    near, mid, last, cosine, sine,
    rq_out, rk_out, v_out, p_out, s1_out, s2_out, s3_out, rows, weight,
):
    y, x, z, c = place[0], place[1], place[2], place[3]
    for shift, part in enumerate((t0, t1, t2, t3)):
        at = lax.rem(x - shift + NX, NX)
        rows[pl.ds(pl.multiple_of(at * SUB, SUB), SUB), :] = part[...]

    def put(part, distance, core, columns):
        at = 2 * lax.rem(z + distance + NZ, NZ) + core
        weight[pl.ds(pl.multiple_of(at * SUB, SUB), SUB), columns] = part

    every, left, right = slice(0, WIDTH), slice(0, WIDTH // 2), slice(WIDTH // 2, WIDTH)
    put(own[...], 0, c, every)
    for n, (fwd, bwd) in enumerate(((f1, b1), (f2, b2), (f3, b3))):
        put(fwd[...], -n - 1, c, every)
        put(bwd[...], n + 1, c, every)
    put(f4[...], 4, c, left)
    put(b4[...], 4, c, right)
    for n, distance in enumerate((0, -1, 1)):
        put(near[n * SUB : (n + 1) * SUB, :], distance, 1 - c, every)
    for n, distance in enumerate((-2, 2, -3, 3)):
        put(mid[n * SUB : (n + 1) * SUB, :], distance, 1 - c, every)
    put(last[...], 4, 1 - c, every)

    half = DK // 2
    row = lax.broadcasted_iota(jnp.int32, (128, 128), 0)
    col = lax.broadcasted_iota(jnp.int32, (128, 128), 1)
    first = lax.rem(col, DK) < half
    turn = jnp.where(
        first & (row == col + half), -1.0, jnp.where((~first) & (row == col - half), 1.0, 0.0)
    ).astype(bf16)
    for n, out in enumerate((rq_out, rk_out)):
        part = dot(rows[...], weight[:, n * GROUP * DK : (n + 1) * GROUP * DK]).astype(bf16)
        for pair in range(GROUP // 2):
            two = part[:, pair * 128 : (pair + 1) * 128]
            turned = two.astype(f32) * cosine[...] + dot(two, turn) * sine[...]
            out[:, pair * 128 : (pair + 1) * 128] = turned.astype(bf16)
    for pair in range(GROUP // 2):
        at = 2 * GROUP * DK + pair * 2 * DV
        v_out[:, pair * 2 * DV : (pair + 1) * 2 * DV] = dot(
            rows[...], weight[:, at : at + 2 * DV]
        ).astype(bf16)

    spot = row.astype(f32)
    for pair in range(GROUP // 2):
        lanes = slice(pair * 128, (pair + 1) * 128)
        slot = [lax.rem(y - (2 * pair + h) + NY, NY) for h in range(2)]
        rate_f = jnp.where(col < DK, rates[0, slot[0]], rates[0, slot[1]])
        rate_b = jnp.where(col < DK, rates[1, slot[0]], rates[1, slot[1]])
        fade_f = jnp.exp(rate_f * (SUB - 1.0 - spot))
        fade_b = jnp.exp(rate_b * spot)
        local = []
        for chunk in range(CHUNKS):
            at = slice(chunk * SUB, (chunk + 1) * SUB)
            keys = rk_out[at, lanes].astype(f32)
            two = v_out[at, pair * 2 * DV : (pair + 1) * 2 * DV]
            local.append(
                tuple(
                    dot((keys * fade).astype(bf16), two, (((0,), (0,)), ((), ())))
                    for fade in (fade_f, fade_b)
                )
            )
        for h in range(2):
            over, along = slice(h * DK, (h + 1) * DK), slice(h * DV, (h + 1) * DV)
            into = slice((2 * pair + h) * DK, (2 * pair + h + 1) * DK)
            step_f = jnp.exp(jnp.full((DK, DV), SUB * rates[0, slot[h]], f32))
            step_b = jnp.exp(jnp.full((DK, DV), SUB * rates[1, slot[h]], f32))
            fwd = jnp.zeros((DK, DV), f32)
            bwd = jnp.zeros((DK, DV), f32)
            for chunk in range(CHUNKS):
                p_out[chunk, into, 0:DV] = fwd
                fwd = fwd * step_f + local[chunk][0][over, along]
                back = CHUNKS - 1 - chunk
                p_out[back, into, DV : 2 * DV] = bwd
                bwd = bwd * step_b + local[back][1][over, along]
            for shift, out in ((1, s1_out), (2, s2_out), (3, s3_out)):
                out[into, :] = jnp.where(y + shift < NY, fwd, bwd).astype(bf16)


def retain_kernel(
    place, rates, rq, rk, values, prefix, r1, r2, r3, w0, w1, w2, w3, other, mine, theirs, normed, *, shift
):
    y, x = place[0], place[1]
    at = lax.rem(x + shift, NX)
    rows = pl.ds(pl.multiple_of(at * SUB, SUB), SUB)
    here = at.astype(f32)
    row = lax.broadcasted_iota(jnp.int32, (SUB, SUB), 0).astype(f32)
    gap = row - lax.broadcasted_iota(jnp.int32, (SUB, SUB), 1).astype(f32)
    for h in range(GROUP):
        slot = lax.rem(y - h + NY, NY)
        rate_f, rate_b = rates[0, slot], rates[1, slot]
        decay = jnp.exp(jnp.where(gap >= 0.0, rate_f * gap, -rate_b * gap))
        decay = jnp.where(gap == 0.0, 2.0, decay)
        query = rq[rows, h * DK : (h + 1) * DK]
        key = rk[rows, h * DK : (h + 1) * DK]
        scores = (dot(query, key, (((1,), (1,)), ((), ()))) * decay).astype(bf16)
        result = dot(scores, values[rows, h * DV : (h + 1) * DV])
        over = slice(h * DK, (h + 1) * DK)
        state_f = prefix[at, over, 0:DV]
        state_b = prefix[at, over, DV : 2 * DV]
        for k, got in ((1, r1), (2, r2), (3, r3)):
            state = got[over, :].astype(f32)
            power = jnp.where(
                y >= k,
                rate_f * (BLOCK * (k - 1.0) + SUB * here),
                rate_b * (BLOCK * (3.0 - k) + SUB * (CHUNKS - 1.0 - here)),
            )
            state = state * jnp.exp(jnp.full((DK, DV), power, f32))
            state_f += jnp.where(y >= k, state, 0.0)
            state_b += jnp.where(y >= k, 0.0, state)
        result += jnp.exp(rate_f * (row + 1.0)) * dot(query, state_f.astype(bf16))
        result += jnp.exp(rate_b * (SUB - row)) * dot(query, state_b.astype(bf16))
        average = jnp.mean(result, axis=-1, keepdims=True)
        centred = result - average
        variance = jnp.mean(centred * centred, axis=-1, keepdims=True)
        normed[h] = (centred * lax.rsqrt(variance + 1e-06)).astype(bf16)
    slots = [lax.rem(y - k + NY, NY) for k in range(NY)]
    total = dot(normed[slots[0]], w0[...])
    for slot, weight in zip(slots[1:], (w1, w2, w3)):
        total += dot(normed[slot], weight[...])
    mine[...] = total.astype(mine.dtype)
    total = dot(normed[slots[0]], other[0:SUB, :])
    for k in range(1, NY):
        total += dot(normed[slots[k]], other[k * SUB : (k + 1) * SUB, :])
    theirs[...] = total.astype(theirs.dtype)


def join_kernel(place, *refs):
    c, out = place[3], refs[-1]
    width = out.shape[1] // 2
    for n, at in ((0, c), (1, 1 - c)):
        parts = [ref[...].astype(f32) for ref in refs[3 * n : 3 * n + 3]]
        along = pl.ds(pl.multiple_of(at * width, 128), width)
        out[:, along] = (parts[0] + parts[1] + parts[2]).astype(bf16)


def shards(tokens, query_weight, key_weight, value_weight, output_weight, log_decay):
    y, x, z, c = (lax.axis_index(a) for a in ("y", "x", "z", "c"))
    place = jnp.stack([y, x, z, c]).astype(jnp.int32)
    half = DK // 2
    frequency = 10000.0 ** (-(jnp.arange(128) % half).astype(f32) / half)
    positions = (y * BLOCK + jnp.arange(BLOCK)).astype(f32)
    angles = positions[:, None] * frequency[None, :]
    cosine, sine = jnp.cos(angles), jnp.sin(angles)
    t0 = tokens[0]
    t1, t3, t2 = (by_shift(t0, "x", k) for k in (1, 3, 2))

    weights = (query_weight, key_weight, value_weight, output_weight)
    own, out_rows = pl.pallas_call(
        pack_kernel,
        out_shape=[
            pltpu.VMEM((SUB, WIDTH), bf16),
            pltpu.VMEM((SUB, output_weight.shape[1] // 2), bf16),
        ],
        in_specs=[SM, ANY, ANY, ANY, ANY],
        out_specs=[VM] * 2,
        scratch_shapes=[pltpu.VMEM((SUB, GROUP * 128), bf16)] * 3 + [pltpu.SemaphoreType.DMA((13,))],
        compiler_params=pltpu.CompilerParams(vmem_limit_bytes=8 * 2**20),
        name="pack",
    )(place, *(pltpu.with_memory_space_constraint(w, pltpu.HBM) for w in weights))
    fwd, bwd, half = [own], [own], WIDTH // 2
    for n in range(1, 4):
        fwd.append(by_shift(fwd[-1], "z", 1))
        bwd.append(by_shift(bwd[-1], "z", -1))
        if n == 1:
            bwd[1], cosine, sine = lax.optimization_barrier((bwd[1], cosine, sine))
    fwd.append(by_shift(fwd[-1][:, :half], "z", 1))
    bwd.append(by_shift(bwd[-1][:, half:], "z", -1))
    mine = [own] + [a for n in range(1, 5) for a in (fwd[n], bwd[n])]
    theirs = [
        swap_cores(jnp.concatenate(parts, axis=axis))
        for axis, parts in (
            (0, (own, fwd[1], bwd[1])), (0, (fwd[2], bwd[2], fwd[3], bwd[3])), (1, (fwd[4], bwd[4]))
        )
    ]

    got = out_rows_fetch(out_rows_spread(out_rows))
    w1, w3, w2 = (by_shift(got, "y", k) for k in (1, 3, 2))
    other = swap_cores(jnp.concatenate([got, w1, w2, w3]))

    rates = jnp.concatenate([log_decay, by_shift(log_decay, "y", 1)], axis=1)
    rates = jnp.concatenate([rates, by_shift(rates, "y", 2)], axis=1)

    state = pltpu.VMEM((GROUP * DK, DV), bf16)
    rq, rk, values, prefix, s1, s2, s3 = pl.pallas_call(
        project_kernel,
        out_shape=(
            pltpu.VMEM((BLOCK, GROUP * DK), bf16),
            pltpu.VMEM((BLOCK, GROUP * DK), bf16),
            pltpu.VMEM((BLOCK, GROUP * DV), bf16),
            pltpu.VMEM((CHUNKS, GROUP * DK, 2 * DV), f32),
            state, state, state,
        ),
        in_specs=[SM, SM] + [VM] * 18,
        out_specs=[VM] * 7,
        scratch_shapes=[
            pltpu.VMEM((BLOCK, t0.shape[1]), bf16),
            pltpu.VMEM((t0.shape[1], WIDTH), bf16),
        ],
        compiler_params=pltpu.CompilerParams(vmem_limit_bytes=24 * 2**20),
        name="project",
    )(place, rates, *in_vmem(t0, t1, t2, t3, *mine, *theirs, cosine, sine))
    r1, r2, r3 = (by_shift(s, "y", k) for k, s in ((1, s1), (2, s2), (3, s3)))

    def part_for(shift, kind):
        return pl.pallas_call(
            functools.partial(retain_kernel, shift=shift),
            out_shape=[pltpu.VMEM((SUB, output_weight.shape[1] // 2), kind)] * 2,
            in_specs=[SM, SM] + [VM] * 12,
            out_specs=[VM] * 2,
            scratch_shapes=[pltpu.VMEM((GROUP, SUB, DV), bf16)],
            compiler_params=pltpu.CompilerParams(vmem_limit_bytes=16 * 2**20),
            name="retain",
        )(place, rates, *in_vmem(rq, rk, values, prefix, r1, r2, r3, got, w1, w2, w3, other))

    far_left, far_right = part_for(2, bf16)
    by_left = by_shift(far_left, "x", 1)
    by_right = by_shift(far_right, "x", -1)
    next_left, next_right = part_for(1, bf16)
    from_right = by_shift(next_right, "x", 1)
    last_left, last_right = part_for(3, bf16)
    from_left = by_shift(last_left, "x", -1)
    own_left, own_right = part_for(0, f32)
    from_left2 = by_shift((next_left.astype(f32) + by_left.astype(f32)).astype(bf16), "x", 1)
    from_right2 = by_shift((last_right.astype(f32) + by_right.astype(f32)).astype(bf16), "x", -1)
    out = pl.pallas_call(
        join_kernel,
        out_shape=jax.ShapeDtypeStruct(t0.shape, bf16),
        in_specs=[SM] + [VM] * 6,
        out_specs=VM,
        compiler_params=pltpu.CompilerParams(vmem_limit_bytes=8 * 2**20),
        name="join",
    )(place, *in_vmem(own_left, from_left, from_left2, own_right, from_right, from_right2))
    return out[None]


def solution(mesh):
    finer = Mesh(mesh.devices.reshape(NY, NX, NZ, 2), ("y", "x", "z", "c"))
    dp, sp = ("z", "c"), ("y", "x")
    placed = (P(dp, sp, None), P(dp, None), P(dp, None), P(dp, None), P(dp, None), P(None, sp))

    return jax.shard_map(shards, mesh=finer, in_specs=placed, out_specs=P(dp, sp, None), check_vma=False)
```
